256 devices in a mesh: grp: 2 (over y), ep: 64 (over z, x), tp: 2 (over core).
Axes of the slice: x: 4, y: 2, z: 16, core: 2. Of those that a mesh axis runs over, the one named last changes fastest.
The devices are a block of a 4x16x16 slice.
Arguments:
- tokens: bfloat16 [65536, 2048], P(('grp', 'ep', 'tp')), parts along dimension 0, may hold values from -15 to 15
- gain_in: float32 [2048], replicated, may hold values from 0.1 to 1.9
- expert_ids: int32 [65536, 2], P(('grp', 'ep')), parts along dimension 0, may hold values from 0 to 63, all different within a row; in each aligned block of 256 rows (0 to 255, 256 to 511, ...) at most 16 rows name the same one
- gate_weights: float32 [65536, 2], P(('grp', 'ep')), parts along dimension 0, may hold values from 0.1 to 1
- w_gate: bfloat16 [64, 2048, 512], P('ep', None, 'tp'), may hold values from -0.125 to 0.125
- w_up: bfloat16 [64, 2048, 512], P('ep', None, 'tp'), may hold values from -0.125 to 0.125
- w_down: bfloat16 [64, 2048, 512], P('ep', None, 'tp'), may hold values from -20 to 20
- gain_out: float32 [2048], P('tp'), may hold values from 0.1 to 1.9
Outputs:
- mixed: bfloat16 [65536, 2048], P(('grp', 'ep'), 'tp'), parts along dimension 0
The draws below stay inside these ranges and needn't reach their ends.
There are 2 independent parts, one for each index of `grp`. The reference program is written for one: setup_inputs(seed, part) draws one part's arguments, and reference() takes and returns one part's arrays. A program takes and returns all parts, laid end to end along the dimension named above; an argument that names none is the same for every part. Nothing has to cross between parts.
Inputs may be any that keep to these rules, and one draw needn't show every extreme that they name: `expert_ids`: each token names 2 different experts; in each aligned block of 256 tokens no expert is named by more than 16 pairs, a bound that some block reaches.
All inputs are finite; a program needn't handle non-finite values.
Results may differ from the reference program's by a relative error of at most 0.0077.
Values may be sent and summed in bfloat16 or wider, within the bound.
No kernel may reach another device: no remote copies, remote signals or barrier semaphores. Data moves between devices by JAX's collectives and lax.ppermute only.
A program may use at most 64 MiB of HBM per device.

```python
import math
import jax
import jax.numpy as jnp
import numpy as np
from jax import lax

D = 2048
DE = 512
TOP_K = 2
TOK_DEV = 256
EXPERTS = 64
CAP = 16
HALVES = 2
TOKENS = 32768


def draw_w_down(key, part):
    jitter = jax.random.uniform(jax.random.fold_in(key, 12), (D,), jnp.float32, 0.6, 1.4)
    column = jnp.arange(D, dtype=jnp.float32) / D
    base = jnp.clip(jax.random.normal(jax.random.fold_in(key, 11), (EXPERTS, D, DE), jnp.float32), -4.0, 4.0)
    rise = 10.0 ** column
    values = base * (rise * jitter)[None, :, None] * DE ** (-0.5)
    return jnp.clip(values, -20.0, 20.0).astype(jnp.bfloat16)


def block_levels(rng, shape, pieces, smallest, top_value):
    gain = 1.0
    for dim, blocks in pieces:
        steps = jax.random.uniform(jax.random.fold_in(jax.random.fold_in(rng, 6), dim), (blocks,), jnp.float32, smallest / len(pieces), top_value / len(pieces))
        gain = gain * jnp.repeat(jnp.exp(steps), shape[dim] // blocks).reshape((-1,) + (1,) * (len(shape) - 1 - dim))
    return gain


def assign_block(stream_key, own, number, rows, number_of, top, reach, slope):
    sequence = jax.random.permutation(stream_key, number_of)
    heavy_load, ordinary = shares(number_of, rows * top, reach, slope, True), shares(number_of, rows * top, reach, slope, False)
    places = jnp.arange(number_of)

    def named(sizes, offset_by):
        used = int((sizes > 0).sum())
        fixed = max(1, used // 4)
        moved = fixed + (places - fixed + offset_by * (used - fixed)) % max(1, number_of - fixed)
        return jnp.zeros((number_of,), jnp.int32).at[sequence[jnp.where(places < fixed, places, moved)]].set(jnp.asarray(sizes, jnp.int32))

    sizes = jnp.where(number % 4 == 0, named(heavy_load, number // 4), named(ordinary, number - number // 4 - 1))
    mixed = jax.random.permutation(jax.random.fold_in(own, 3), number_of)
    source_of, receiver = mixed[0:number_of // 2 * 2:2], mixed[1:number_of // 2 * 2:2]
    room = jnp.minimum(sizes[source_of] - 1, reach - sizes[receiver]) // 2
    room = jnp.where((source_of == sequence[0]) | (receiver == sequence[0]) | (sizes[receiver] == 0), 0, jnp.maximum(room, 0))
    moved = jax.random.randint(jax.random.fold_in(own, 4), (number_of // 2,), 0, 1 << 20) % (room + 1)
    sizes = sizes.at[source_of].add(-moved).at[receiver].add(moved)
    items = jnp.searchsorted(jnp.cumsum(sizes), jnp.arange(rows * top), side="right").astype(jnp.int32)
    table = items.reshape(top, rows).T
    table = table[jax.random.permutation(jax.random.fold_in(own, 1), rows)]
    offset_by = jax.random.randint(jax.random.fold_in(own, 2), (rows, 1), 0, top)
    return jnp.take_along_axis(table, (jnp.arange(top)[None, :] + offset_by) % top, axis=1)


def shares(amount, total, most, lean, full):
    portions = [(1 << 20) // math.isqrt(grade ** lean) + 1 for grade in range(1, amount + 1)]
    largest = most if full else min(most, max(-(-total // amount), total * portions[0] // sum(portions)))
    least = 1 if total - largest >= amount - 1 else 0
    given, spare = [largest] + [least] * (amount - 1), total - largest - least * (amount - 1)
    while spare > 0:
        movable = [i for i in range(1, amount) if given[i] < largest] or [i for i in range(1, amount) if given[i] < most]
        whole, left = sum([portions[i] for i in movable]), spare
        for i in movable:
            addition = min(most - given[i], max(1, left * portions[i] // whole), spare)
            given[i] = given[i] + addition
            spare = spare - addition
    return np.array(given)


def gaussian(rng, dims, spread, most, shards=(), kind=jnp.bfloat16):
    result = jax.random.normal(rng, dims, jnp.float32) * spread
    if len(shards) > 0:
        result = block_levels(rng, dims, shards, -0.22, 0.18) * result
    return jnp.clip(result, min=-most, max=most).astype(kind)


def setup_inputs(seed: int = 0, part: int = 0) -> dict:
    seeds = jax.random.split(jax.random.key(seed), 9)
    part_splits = jax.random.split(jax.random.fold_in(seeds[8], part), 9)
    tokens = gaussian(part_splits[0], (TOKENS, D), 3.0, 15.0, ((0, 128),))
    gain_in = jnp.clip(1.0 + 0.18 * jax.random.normal(seeds[1], (D,), jnp.float32), 0.1, 1.9)
    expert_ids_keys = jax.random.split(jax.random.fold_in(part_splits[2], 1), TOKENS // TOK_DEV)
    expert_ids_turns = jax.random.permutation(jax.random.fold_in(part_splits[2], 3), TOKENS // TOK_DEV)
    expert_ids = jax.vmap(lambda own, number: assign_block(jax.random.fold_in(part_splits[2], 2), own, number, TOK_DEV, EXPERTS, TOP_K, CAP, 2))(expert_ids_keys, expert_ids_turns).reshape((TOKENS, TOP_K))
    gate_weights = jnp.clip(jnp.exp(math.log(1.0) - 2.3025851 * jax.random.uniform(part_splits[3], (TOKENS, TOP_K), jnp.float32) ** block_levels(part_splits[3], (TOKENS, TOP_K), ((0, 64),), -0.2, 0.2)), 0.1, 1.0)
    w_gate = gaussian(seeds[4], (EXPERTS, D, DE), D ** -0.5, 0.125, ((0, 64), (2, 2)))
    w_up = gaussian(seeds[5], (EXPERTS, D, DE), D ** -0.5, 0.125, ((0, 64), (2, 2)))
    w_down = draw_w_down(jax.random.fold_in(seeds[8], 71), part)
    gain_out = jnp.clip(1.0 + 0.18 * jax.random.normal(seeds[7], (D,), jnp.float32), 0.1, 1.9)
    return dict(tokens=tokens, gain_in=gain_in, expert_ids=expert_ids, gate_weights=gate_weights, w_gate=w_gate, w_up=w_up, w_down=w_down, gain_out=gain_out)


EPS = 1e-06

def block_slots(expert_ids, block_rows, experts):
    pairs = expert_ids.reshape(-1, block_rows * expert_ids.shape[1])
    onehot = (pairs[:, :, None] == jnp.arange(experts, dtype=jnp.int32)[None, None, :]).astype(jnp.int32)
    before = jnp.cumsum(onehot, axis=1) - onehot
    return lax.optimization_barrier(jnp.sum(before * onehot, axis=2)).reshape(expert_ids.shape).astype(jnp.int32)

def reference(tokens, gain_in, expert_ids, gate_weights, w_gate, w_up, w_down, gain_out):
    x_float = tokens.astype(jnp.float32)
    normed = (x_float * lax.rsqrt(lax.optimization_barrier(jnp.mean(x_float * x_float, axis=1, keepdims=True)) + EPS) * gain_in).astype(jnp.bfloat16)
    slots = block_slots(expert_ids, TOK_DEV, EXPERTS)
    sources = TOKENS // TOK_DEV
    token_ids = jnp.broadcast_to(jnp.arange(TOKENS, dtype=jnp.int32)[:, None], expert_ids.shape)
    position = token_ids // TOK_DEV * CAP + slots
    table = jnp.full((EXPERTS, sources * CAP), TOKENS, jnp.int32).at[expert_ids, position].set(token_ids)
    row_gates = jnp.zeros((EXPERTS, sources * CAP), jnp.float32).at[expert_ids, position].set(gate_weights)
    padded = jnp.concatenate([normed, jnp.zeros((1, D), jnp.bfloat16)], axis=0)
    block = DE // HALVES

    def one_expert(total, inputs):
        rows_index, gates_here, gate_matrix, up_matrix, down_matrix = inputs
        rows = padded[rows_index]
        gated = jnp.dot(rows, gate_matrix, preferred_element_type=jnp.float32)
        upward = jnp.dot(rows, up_matrix, preferred_element_type=jnp.float32)
        hidden = (jax.nn.silu(gated) * upward).astype(jnp.bfloat16)
        summed = jnp.zeros((rows.shape[0], D), jnp.float32)
        for index in range(HALVES):
            part = lax.dot_general(hidden[:, index * block:(index + 1) * block], down_matrix[:, index * block:(index + 1) * block], (((1,), (1,)), ((), ())), preferred_element_type=jnp.float32)
            summed = summed + lax.optimization_barrier(part.astype(jnp.bfloat16)).astype(jnp.float32)
        expert_out = summed.astype(jnp.bfloat16).astype(jnp.float32)
        return (total.at[rows_index].add(gates_here[:, None] * expert_out), None)
    combined, _ = lax.scan(one_expert, jnp.zeros((TOKENS + 1, D), jnp.float32), (table, row_gates, w_gate, w_up, w_down))
    combined = combined[:TOKENS]
    inverse = lax.rsqrt(lax.optimization_barrier(jnp.mean(combined * combined, axis=1, keepdims=True)) + EPS)
    return (combined * inverse * gain_out).astype(jnp.bfloat16)
```

```python
import jax
import jax.numpy as jnp
from jax import lax
from jax.sharding import PartitionSpec as P

EPS = 1e-06
SIDE = 4
PARTS = 2
HEAD = 8
BATCHES = ((0, 1, 2), (3, 4), (5, 6), (7, 8))
BF = jnp.bfloat16
F32 = jnp.float32


def dot(a, b, out=F32):
    return jnp.dot(a, b, preferred_element_type=F32).astype(out)


def dot_t(a, b):
    return lax.dot_general(a, b, (((0,), (0,)), ((), ())), preferred_element_type=F32)


def rms(x):
    return lax.rsqrt(jnp.mean(x * x, axis=1, keepdims=True) + EPS)


def pair_slots(experts_of):
    number = experts_of.shape[0]
    same = experts_of[:, None] == experts_of[None, :]
    earlier = jnp.arange(number)[:, None] > jnp.arange(number)[None, :]
    return jnp.sum((same & earlier).astype(jnp.int32), axis=1)


def far_first(reach):
    number = reach.shape[0]
    order = jnp.arange(number)
    ahead = (reach[None, :] > reach[:, None]) | (
        (reach[None, :] == reach[:, None]) & (order[None, :] < order[:, None])
    )
    return jnp.sum(ahead.astype(jnp.int32), axis=1)


def onehot_rows(index, number, offset):
    return (index[:, None] == (jnp.arange(number) - offset).astype(F32)[None, :]).astype(BF)


def per_device(tokens, gain_in, expert_ids, gate_weights, w_gate, w_up, w_down, gain_out):
    rows, width = tokens.shape
    top = expert_ids.shape[1]
    members = lax.axis_size("ep")
    planes = members // SIDE
    half = planes // 2
    experts = w_gate.shape[0] * members
    capacity = 2 * rows * top // experts
    entries = SIDE * capacity
    part = width // PARTS

    def along_z(step):
        return [(i, ((i // SIDE + step) % planes) * SIDE + i % SIDE) for i in range(members)]

    def along_x(step):
        return [(i, (i // SIDE) * SIDE + (i % SIDE + step) % SIDE) for i in range(members)]

    bound = [min(rows, entries * (half - h) + entries // 2) for h in range(1, half + 1)]

    me = lax.axis_index("ep")
    core = lax.axis_index("tp")
    my_z, my_x = me // SIDE, me % SIDE

    ids = lax.dynamic_slice_in_dim(expert_ids, core * rows, rows, 0)
    gates = lax.dynamic_slice_in_dim(gate_weights, core * rows, rows, 0)
    flat = ids.reshape(-1)
    slot = pair_slots(flat)
    ahead = jnp.mod(flat // SIDE - my_z, planes)
    beside = jnp.mod(flat % SIDE - my_x, SIDE)
    upper = slot < capacity // 2
    up_reach = jnp.where((ahead < half) | ((ahead == half) & upper), ahead, 0)
    down_reach = jnp.where((ahead > half) | ((ahead == half) & ~upper), planes - ahead, 0)
    ranks = [far_first(jnp.max(r.reshape(rows, top), axis=1)) for r in (up_reach, down_reach)]
    column = ahead * entries + beside * capacity + slot
    flat_gates = gates.reshape(-1)
    gate_hi = flat_gates.astype(BF)
    gate_lo = (flat_gates - gate_hi.astype(F32)).astype(BF)
    values = jnp.stack(
        [jnp.repeat(r, top).astype(BF) for r in (ranks[0], ranks[1], jnp.arange(rows))]
        + [gate_hi, gate_lo, jnp.ones_like(gate_hi)],
        axis=1,
    )
    chosen = (jnp.arange(planes * entries)[:, None] == column[None, :]).astype(BF)
    table = dot(chosen, values).reshape(planes, entries, values.shape[1])
    filled = table[:, :, 5] > 0
    low_slot = (jnp.arange(entries) % capacity) < capacity // 2

    def header(direction):
        planes_of = [h if direction == 0 else planes - h for h in range(1, half + 1)]
        index = jnp.stack([table[p, :, direction] for p in planes_of])
        ok = jnp.stack([filled[p] for p in planes_of])
        last = low_slot if direction == 0 else ~low_slot
        ok = ok.at[half - 1].set(ok[half - 1] & last)
        index = jnp.where(ok, index, -1.0)
        hi = jnp.stack([table[p, :, 3] for p in planes_of])
        lo = jnp.stack([table[p, :, 4] for p in planes_of])
        data = jnp.stack([index.reshape(-1), hi.reshape(-1), lo.reshape(-1)]).astype(BF)
        return jnp.pad(data, ((0, HEAD - 3), (0, part - data.shape[1])))

    x_float = tokens.astype(F32)
    normed = (x_float * rms(x_float) * gain_in).astype(BF)

    orders = [(jnp.arange(rows)[:, None] == r[None, :]).astype(BF) for r in ranks]
    buffers = []
    for d in (0, 1):
        ordered = dot(orders[d], normed, BF)
        pieces = [ordered[:, p * part : (p + 1) * part] for p in range(PARTS)]
        pieces[0] = jnp.concatenate([header(d), pieces[0]], axis=0)
        buffers.append(pieces)

    swap = [(0, 1), (1, 0)]
    gate_all = jnp.concatenate([w_gate[0], lax.ppermute(w_gate, "tp", swap)[0]], axis=1)
    up_all = jnp.concatenate([w_up[0], lax.ppermute(w_up, "tp", swap)[0]], axis=1)
    down_all = jnp.concatenate([w_down[0], lax.ppermute(w_down, "tp", swap)[0]], axis=1)

    def expert(arrived):
        hidden = (jax.nn.silu(dot(arrived, gate_all)) * dot(arrived, up_all)).astype(BF)
        return lax.dot_general(
            hidden, down_all, (((1,), (1,)), ((), ())), preferred_element_type=F32
        ).astype(BF)

    own_index = jnp.where(filled[0], table[0, :, 2], -1.0)
    routes = {(0, 0): (own_index, table[0, :, 3], table[0, :, 4])}
    picked = {0: [dot(onehot_rows(own_index, rows, 0), normed, BF)]}
    for h in range(1, half + 1):
        here = []
        for d in (0, 1):
            step = 1 if d == 0 else -1
            got = []
            for p in range(PARTS):
                take = bound[h - 1] + (HEAD if p == 0 else 0)
                got.append(lax.ppermute(buffers[d][p][:take], "ep", along_z(step)))
            buffers[d] = got
            mine = got[0][:3, (h - 1) * entries : h * entries].astype(F32)
            routes[(h, d)] = (mine[0], mine[1], mine[2])
            rows_here = [
                dot(onehot_rows(mine[0], got[p].shape[0], HEAD if p == 0 else 0), got[p], BF)
                for p in range(PARTS)
            ]
            here.append(jnp.concatenate(rows_here, axis=1))
        picked[h] = [here[0] + here[1]] if h == half else here

    answers = {}
    for batch in BATCHES:
        sources = jnp.stack([r for h in batch for r in picked[h]])
        count = sources.shape[0]
        sources = sources.reshape(count, SIDE, capacity, width)
        sent = [
            sources[:, j].reshape(count * capacity, width)
            if j == 0
            else lax.ppermute(sources[:, j].reshape(count * capacity, width), "ep", along_x(j))
            for j in range(SIDE)
        ]
        result = expert(jnp.concatenate(sent, axis=0)).reshape(SIDE, count * capacity, width)
        back = [
            result[j] if j == 0 else lax.ppermute(result[j], "ep", along_x(-j)) for j in range(SIDE)
        ]
        at = 0
        for h in batch:
            answers[h] = []
            for _ in picked[h]:
                answers[h].append(
                    jnp.concatenate([b[at * capacity : (at + 1) * capacity] for b in back], axis=0)
                )
                at += 1

    def weighted(route, number):
        index, hi, lo = route
        hot = index[:, None] == jnp.arange(number).astype(F32)[None, :]
        return jnp.concatenate(
            [jnp.where(hot, hi[:, None], 0.0), jnp.where(hot, lo[:, None], 0.0)], axis=0
        ).astype(BF)

    carried = [[None] * PARTS, [None] * PARTS]
    for h in range(half, 0, -1):
        for d in (0, 1):
            step = -1 if d == 0 else 1
            answer = answers[h][0] if h == half else answers[h][d]
            twice = jnp.concatenate([answer, answer], axis=0)
            spread = weighted(routes[(h, d)], bound[h - 1])
            for p in range(PARTS):
                local = dot_t(spread, twice[:, p * part : (p + 1) * part])
                if carried[d][p] is not None:
                    extra = bound[h - 1] - carried[d][p].shape[0]
                    local = local + jnp.pad(carried[d][p].astype(F32), ((0, extra), (0, 0)))
                carried[d][p] = lax.ppermute(local.astype(BF), "ep", along_z(step))

    own = answers[0][0]
    final = jnp.concatenate([orders[0], orders[1], weighted(routes[(0, 0)], rows)], axis=0)
    outs = []
    for p in range(PARTS):
        piece = own[:, p * part : (p + 1) * part]
        outs.append(
            dot_t(final, jnp.concatenate([carried[0][p], carried[1][p], piece, piece], axis=0))
        )
    combined = jnp.concatenate(outs, axis=1)
    scaled = (combined * rms(combined)).astype(BF)
    share = width // 2
    keep = lax.dynamic_slice_in_dim(scaled, core * share, share, 1)
    give = lax.dynamic_slice_in_dim(scaled, (1 - core) * share, share, 1)
    got = lax.ppermute(give, "tp", swap)
    first = jnp.where(core == 0, keep, got)
    second = jnp.where(core == 0, got, keep)
    both = jnp.concatenate([first, second], axis=0).astype(F32)
    return (both * gain_out).astype(BF)


def solution(mesh):
    placed = (
        P(("grp", "ep", "tp"), None),
        P(),
        P(("grp", "ep"), None),
        P(("grp", "ep"), None),
        P("ep", None, "tp"),
        P("ep", None, "tp"),
        P("ep", None, "tp"),
        P("tp"),
    )
    return jax.shard_map(
        per_device, mesh=mesh, in_specs=placed, out_specs=P(("grp", "ep"), "tp"), check_vma=False
    )
```

```python
import jax
import jax.numpy as jnp
from jax import lax
from jax.experimental import pallas as pl
from jax.experimental.pallas import tpu as pltpu
from jax.sharding import PartitionSpec as P


EPS = 1e-06
SIDE = 4
PARTS = 2
HEAD = 8
BATCHES = ((5, 6, 7, 8), (0, 1, 2, 3, 4))
BF = jnp.bfloat16
F32 = jnp.float32


def dot(a, b, out=F32):
    return jnp.dot(a, b, preferred_element_type=F32).astype(out)


def dot_t(a, b):
    return lax.dot_general(a, b, (((0,), (0,)), ((), ())), preferred_element_type=F32)


def rms(x):
    return lax.rsqrt(jnp.mean(x * x, axis=1, keepdims=True) + EPS)


def pair_slots(experts_of):
    number = experts_of.shape[0]
    same = experts_of[:, None] == experts_of[None, :]
    earlier = jnp.arange(number)[:, None] > jnp.arange(number)[None, :]
    return jnp.sum((same & earlier).astype(jnp.int32), axis=1)


def far_first(reach):
    number = reach.shape[0]
    order = jnp.arange(number)
    ahead = (reach[None, :] > reach[:, None]) | (
        (reach[None, :] == reach[:, None]) & (order[None, :] < order[:, None])
    )
    return jnp.sum(ahead.astype(jnp.int32), axis=1)


def onehot_rows(index, number, offset):
    return (index[:, None] == (jnp.arange(number) - offset).astype(F32)[None, :]).astype(BF)


def plane_experts(sources, weights, capacity, width):
    count = len(sources)
    entries = SIDE * capacity
    shapes = [[len(parts) for _, parts in source] for source in sources]
    operands = [a for source in sources for pick, parts in source for a in (pick, *parts)]
    arrays, pieces = [], []
    for e, pair in enumerate(weights):
        for k, parts in enumerate(pair):
            for i, (array, at) in enumerate(parts):
                known = [n for n, a in enumerate(arrays) if a is array]
                if not known:
                    arrays.append(array)
                pieces.append((2 * e + k, i, known[0] if known else len(arrays) - 1, at))
    hidden = arrays[0].shape[1]
    part_rows = 3 * width // 2

    def body(*refs):
        ins = refs[: len(operands)]
        held = refs[len(operands) : len(operands) + len(arrays)]
        out, store, rows, sems = refs[len(operands) + len(arrays) :]
        for slot, i, n, at in pieces:
            pltpu.make_async_copy(
                held[n].at[at : at + part_rows],
                store.at[slot, i * part_rows : (i + 1) * part_rows],
                sems.at[slot, i],
            ).start()
        at = 0
        for i, source in enumerate(shapes):
            total = None
            for parts in source:
                pick = ins[at][...]
                found = [
                    jnp.dot(pick, ins[at + 1 + p][...], preferred_element_type=F32)
                    for p in range(parts)
                ]
                found = jnp.concatenate(found, axis=1) if parts > 1 else found[0]
                total = found if total is None else total + found
                at += 1 + parts
            total = total.astype(BF)
            for e in range(SIDE):
                rows[e, i * capacity : (i + 1) * capacity, :] = total[
                    e * capacity : (e + 1) * capacity
                ]

        def one_expert(e, carry):
            x = rows[e]
            y = None
            for k in (0, 1):
                slot = 2 * e + k
                for i in (0, 1):
                    pltpu.make_async_copy(
                        held[0].at[:part_rows],
                        store.at[slot, i * part_rows : (i + 1) * part_rows],
                        sems.at[slot, i],
                    ).wait()
                g = jnp.dot(x, store[slot, :width], preferred_element_type=F32)
                u = jnp.dot(x, store[slot, width : 2 * width], preferred_element_type=F32)
                h = (g / (1.0 + jnp.exp(-g)) * u).astype(BF)
                part = lax.dot_general(
                    h,
                    store[slot, 2 * width :],
                    (((1,), (1,)), ((), ())),
                    preferred_element_type=F32,
                )
                y = part if y is None else y + part
            y = y.astype(BF)
            for i in range(count):
                out[i, pl.ds(pl.multiple_of(e * capacity, capacity), capacity), :] = y[
                    i * capacity : (i + 1) * capacity
                ]
            return carry

        lax.fori_loop(0, SIDE, one_expert, 0)

    flops = count * entries * width * hidden * 12
    moved = 2 * width * hidden * 6 * SIDE + sum(a.size * 2 for a in operands)
    return pl.pallas_call(
        body,
        in_specs=[pl.BlockSpec(memory_space=pltpu.VMEM)] * len(operands)
        + [pl.BlockSpec(memory_space=pl.ANY)] * len(arrays),
        out_specs=pl.BlockSpec(memory_space=pltpu.VMEM),
        out_shape=jax.ShapeDtypeStruct((count, entries, width), BF),
        scratch_shapes=[
            pltpu.VMEM((2 * SIDE, 3 * width, hidden), BF),
            pltpu.VMEM((SIDE, count * capacity, width), BF),
            pltpu.SemaphoreType.DMA((2 * SIDE, 2)),
        ],
        compiler_params=pltpu.CompilerParams(vmem_limit_bytes=58 * 2**20),
        cost_estimate=pl.CostEstimate(
            flops=flops, bytes_accessed=moved, transcendentals=count * entries * hidden * 2
        ),
    )(*operands, *arrays)


def per_device(tokens, gain_in, expert_ids, gate_weights, w_gate, w_up, w_down, gain_out):
    rows, width = tokens.shape
    top = expert_ids.shape[1]
    members = lax.axis_size("ep")
    planes = members // SIDE
    half = planes // 2
    experts = w_gate.shape[0] * members
    capacity = 2 * rows * top // experts
    entries = SIDE * capacity
    part = width // PARTS

    def along_z(step):
        return [(i, ((i // SIDE + step) % planes) * SIDE + i % SIDE) for i in range(members)]

    def along_x(step):
        return [(i, (i // SIDE) * SIDE + (i % SIDE + step) % SIDE) for i in range(members)]

    bound = [min(rows, entries * (half - h) + entries // 2) for h in range(1, half + 1)]

    me = lax.axis_index("ep")
    core = lax.axis_index("tp")
    my_z, my_x = me // SIDE, me % SIDE

    ids = lax.dynamic_slice_in_dim(expert_ids, core * rows, rows, 0)
    gates = lax.dynamic_slice_in_dim(gate_weights, core * rows, rows, 0)
    flat = ids.reshape(-1)
    slot = pair_slots(flat)
    ahead = jnp.mod(flat // SIDE - my_z, planes)
    beside = jnp.mod(flat % SIDE - my_x, SIDE)
    upper = slot < capacity // 2
    up_reach = jnp.where((ahead < half) | ((ahead == half) & upper), ahead, 0)
    down_reach = jnp.where((ahead > half) | ((ahead == half) & ~upper), planes - ahead, 0)
    ranks = [far_first(jnp.max(r.reshape(rows, top), axis=1)) for r in (up_reach, down_reach)]
    column = ahead * entries + beside * capacity + slot
    flat_gates = gates.reshape(-1)
    gate_hi = flat_gates.astype(BF)
    gate_lo = (flat_gates - gate_hi.astype(F32)).astype(BF)
    values = jnp.stack(
        [jnp.repeat(r, top).astype(BF) for r in (ranks[0], ranks[1], jnp.arange(rows))]
        + [gate_hi, gate_lo, jnp.ones_like(gate_hi)],
        axis=1,
    )
    chosen = (jnp.arange(planes * entries)[:, None] == column[None, :]).astype(BF)
    table = dot(chosen, values).reshape(planes, entries, values.shape[1])
    filled = table[:, :, 5] > 0
    low_slot = (jnp.arange(entries) % capacity) < capacity // 2

    def header(direction):
        planes_of = [h if direction == 0 else planes - h for h in range(1, half + 1)]
        index = jnp.stack([table[p, :, direction] for p in planes_of])
        ok = jnp.stack([filled[p] for p in planes_of])
        last = low_slot if direction == 0 else ~low_slot
        ok = ok.at[half - 1].set(ok[half - 1] & last)
        index = jnp.where(ok, index, -1.0)
        hi = jnp.stack([table[p, :, 3] for p in planes_of])
        lo = jnp.stack([table[p, :, 4] for p in planes_of])
        data = jnp.stack([index.reshape(-1), hi.reshape(-1), lo.reshape(-1)]).astype(BF)
        return jnp.pad(data, ((0, HEAD - 3), (0, part - data.shape[1])))

    x_float = tokens.astype(F32)
    normed = (x_float * rms(x_float) * gain_in).astype(BF)

    orders = [(jnp.arange(rows)[:, None] == r[None, :]).astype(BF) for r in ranks]
    buffers = []
    for d in (0, 1):
        ordered = dot(orders[d], normed, BF)
        pieces = [ordered[:, p * part : (p + 1) * part] for p in range(PARTS)]
        pieces = [
            jnp.concatenate([header(d) if p == 0 else jnp.zeros((HEAD, part), BF), piece], axis=0)
            for p, piece in enumerate(pieces)
        ]
        buffers.append(pieces)

    swap = [(0, 1), (1, 0)]

    packed = jnp.concatenate([w_gate[0], w_up[0], w_down[0]], axis=0)
    split = packed.shape[0] // 2
    from_left = lax.ppermute(packed, "ep", along_x(1))
    from_right = lax.ppermute(packed, "ep", along_x(-1))
    far_top = lax.ppermute(from_left[:split], "ep", along_x(1))
    far_low = lax.ppermute(from_right[split:], "ep", along_x(-1))
    weights = []
    for array in (packed, from_right, (far_top, far_low), from_left):
        if isinstance(array, tuple):
            mine = [(a, 0) for a in array]
            other = [(lax.ppermute(a, "tp", swap), 0) for a in array]
        else:
            mine = [(array, 0), (array, split)]
            swapped = lax.ppermute(array, "tp", swap)
            other = [(swapped, 0), (swapped, split)]
        weights.append((mine, other))

    own_index = jnp.where(filled[0], table[0, :, 2], -1.0)
    routes = {(0, 0): (own_index, table[0, :, 3], table[0, :, 4])}
    picked = {0: [[(onehot_rows(own_index, rows, 0), [normed])]]}
    for h in range(1, half + 1):
        here = []
        for d in (0, 1):
            step = 1 if d == 0 else -1
            got = []
            for p in range(PARTS):
                take = bound[h - 1] + HEAD
                got.append(lax.ppermute(buffers[d][p][:take], "ep", along_z(step)))
            buffers[d] = got
            mine = got[0][:3, (h - 1) * entries : h * entries].astype(F32)
            routes[(h, d)] = (mine[0], mine[1], mine[2])
            here.append((onehot_rows(mine[0], got[0].shape[0], HEAD), got))
        picked[h] = [here] if h == half else [[one] for one in here]

    answers = {}
    for batch in BATCHES:
        result = plane_experts([s for h in batch for s in picked[h]], weights, capacity, width)
        at = 0
        for h in batch:
            answers[h] = [result[at + i] for i in range(len(picked[h]))]
            at += len(picked[h])

    def weighted(route, number):
        index, hi, lo = route
        hot = index[:, None] == jnp.arange(number).astype(F32)[None, :]
        return jnp.concatenate(
            [jnp.where(hot, hi[:, None], 0.0), jnp.where(hot, lo[:, None], 0.0)], axis=0
        ).astype(BF)

    carried = [[None] * PARTS, [None] * PARTS]
    for h in range(half, 0, -1):
        for d in (0, 1):
            step = -1 if d == 0 else 1
            answer = answers[h][0] if h == half else answers[h][d]
            twice = jnp.concatenate([answer, answer], axis=0)
            spread = weighted(routes[(h, d)], bound[h - 1])
            for p in range(PARTS):
                local = dot_t(spread, twice[:, p * part : (p + 1) * part])
                if carried[d][p] is not None:
                    extra = bound[h - 1] - carried[d][p].shape[0]
                    local = local + jnp.pad(carried[d][p].astype(F32), ((0, extra), (0, 0)))
                carried[d][p] = lax.ppermute(local.astype(BF), "ep", along_z(step))

    own = answers[0][0]
    final = jnp.concatenate([orders[0], orders[1], weighted(routes[(0, 0)], rows)], axis=0)
    outs = []
    for p in range(PARTS):
        piece = own[:, p * part : (p + 1) * part]
        outs.append(
            dot_t(final, jnp.concatenate([carried[0][p], carried[1][p], piece, piece], axis=0))
        )
    combined = jnp.concatenate(outs, axis=1)
    scaled = (combined * rms(combined)).astype(BF)
    share = width // 2
    keep = lax.dynamic_slice_in_dim(scaled, core * share, share, 1)
    give = lax.dynamic_slice_in_dim(scaled, (1 - core) * share, share, 1)
    got = lax.ppermute(give, "tp", swap)
    first = jnp.where(core == 0, keep, got)
    second = jnp.where(core == 0, got, keep)
    both = jnp.concatenate([first, second], axis=0).astype(F32)
    return (both * gain_out).astype(BF)


def solution(mesh):
    placed = (
        P(("grp", "ep", "tp"), None),
        P(),
        P(("grp", "ep"), None),
        P(("grp", "ep"), None),
        P("ep", None, "tp"),
        P("ep", None, "tp"),
        P("ep", None, "tp"),
        P("tp"),
    )

    return jax.shard_map(
        per_device, mesh=mesh, in_specs=placed, out_specs=P(("grp", "ep"), "tp"), check_vma=False
    )
```

```python
import jax
import jax.numpy as jnp
from jax import lax
from jax.experimental import pallas as pl
from jax.experimental.pallas import tpu as pltpu
from jax.sharding import PartitionSpec as P


EPS = 1e-06
SIDE = 4
PARTS = 2
WEIGHTS_IN = pltpu.HBM
NOWHERE = -128.0
HEAD = 8
BATCHES = ((5, 6, 7, 8), (0, 1, 2, 3, 4))
BF = jnp.bfloat16
F32 = jnp.float32


def dot(a, b, out=F32):
    return jnp.dot(a, b, preferred_element_type=F32).astype(out)


def dot_t(a, b):
    return lax.dot_general(a, b, (((0,), (0,)), ((), ())), preferred_element_type=F32)


def rms(x):
    return lax.rsqrt(jnp.mean(x * x, axis=1, keepdims=True) + EPS)


def pair_slots(experts_of):
    number = experts_of.shape[0]
    same = experts_of[:, None] == experts_of[None, :]
    earlier = jnp.arange(number)[:, None] > jnp.arange(number)[None, :]
    return jnp.sum((same & earlier).astype(jnp.int32), axis=1)


def far_first(reach):
    number = reach.shape[0]
    order = jnp.arange(number)
    ahead = (reach[None, :] > reach[:, None]) | (
        (reach[None, :] == reach[:, None]) & (order[None, :] < order[:, None])
    )
    return jnp.sum(ahead.astype(jnp.int32), axis=1)


def plane_experts(sources, weights, capacity, width):
    count = len(sources)
    entries = SIDE * capacity
    lanes = 2 * entries
    operands, layout, results = [], [], []
    for source in sources:
        placed = []
        for routing, distance, parts in source:
            at = len(operands)
            operands.extend(([] if routing is None else [routing]) + list(parts))
            number = parts[-1].shape[0]
            placed.append((at, routing is None, distance, len(parts), number, len(results)))
            results.extend(jax.ShapeDtypeStruct((number, p.shape[1]), BF) for p in parts)
        layout.append(placed)
    arrays, pieces = [], []
    for e, pair in enumerate(weights):
        for k, parts in enumerate(pair):
            for i, (array, at) in enumerate(parts):
                known = [n for n, a in enumerate(arrays) if a is array]
                if not known:
                    arrays.append(array)
                pieces.append((2 * e + k, i, known[0] if known else len(arrays) - 1, at))
    hidden = arrays[0].shape[1]
    part_rows = 3 * width // 2

    def body(*refs):
        ins = refs[: len(operands)]
        held = refs[len(operands) : len(operands) + len(arrays)]
        outs = refs[len(operands) + len(arrays) : -4]
        store, rows, answers, sems = refs[-4:]
        for slot, i, n, at in pieces:
            pltpu.make_async_copy(
                held[n].at[at : at + part_rows],
                store.at[slot, i * part_rows : (i + 1) * part_rows],
                sems.at[slot, i],
            ).start()

        def routed(at, inside, distance, number):
            if inside:
                lane = (distance - 1) * lanes
                head = ins[at][0:HEAD, lane : lane + lanes].astype(F32)
            else:
                head = ins[at][...].astype(F32)
            place = lax.broadcasted_iota(jnp.int32, (number, lanes), 0).astype(F32)
            return head, place == head[0:1]

        for i, source in enumerate(layout):
            total = None
            for at, inside, distance, parts, number, _ in source:
                _, hot = routed(at, inside, distance, number)
                pick = jnp.where(hot, 1.0, 0.0)
                found = []
                for p in range(parts):
                    values = ins[at + (0 if inside else 1) + p]
                    choice = pick
                    if inside and p == 0:
                        choice = jnp.concatenate([jnp.zeros((HEAD, lanes), F32), pick], axis=0)
                    found.append(
                        lax.dot_general(
                            choice.astype(BF),
                            values[...],
                            (((0,), (0,)), ((), ())),
                            preferred_element_type=F32,
                        )[:entries]
                    )
                found = jnp.concatenate(found, axis=1) if parts > 1 else found[0]
                total = found if total is None else total + found
            total = total.astype(BF)
            for e in range(SIDE):
                rows[e, i * capacity : (i + 1) * capacity, :] = total[
                    e * capacity : (e + 1) * capacity
                ]

        def one_expert(e, carry):
            x = rows[e]
            y = None
            for k in (0, 1):
                slot = 2 * e + k
                for i in (0, 1):
                    pltpu.make_async_copy(
                        held[0].at[:part_rows],
                        store.at[slot, i * part_rows : (i + 1) * part_rows],
                        sems.at[slot, i],
                    ).wait()
                g = jnp.dot(x, store[slot, :width], preferred_element_type=F32)
                u = jnp.dot(x, store[slot, width : 2 * width], preferred_element_type=F32)
                h = (g / (1.0 + jnp.exp(-g)) * u).astype(BF)
                part = lax.dot_general(
                    h,
                    store[slot, 2 * width :],
                    (((1,), (1,)), ((), ())),
                    preferred_element_type=F32,
                )
                y = part if y is None else y + part
            y = y.astype(BF)
            for i in range(count):
                mine = y[i * capacity : (i + 1) * capacity]
                for base in (0, entries):
                    first = pl.multiple_of(base + e * capacity, capacity)
                    answers[i, pl.ds(first, capacity), :] = mine
            return carry

        lax.fori_loop(0, SIDE, one_expert, 0)

        for i, source in enumerate(layout):
            for at, inside, distance, parts, number, to in source:
                head, hot = routed(at, inside, distance, number)
                spread = jnp.where(hot, head[1:2], 0.0).astype(BF)
                lane = 0
                for p in range(parts):
                    span = outs[to + p].shape[1]
                    outs[to + p][...] = jnp.dot(
                        spread, answers[i, :, lane : lane + span], preferred_element_type=F32
                    ).astype(BF)
                    lane += span

    flops = count * entries * width * hidden * 12
    moved = 2 * width * hidden * 6 * SIDE + sum(a.size * 4 for a in operands)
    made = pl.pallas_call(
        body,
        in_specs=[pl.BlockSpec(memory_space=pltpu.VMEM)] * len(operands)
        + [pl.BlockSpec(memory_space=WEIGHTS_IN)] * len(arrays),
        out_specs=[pl.BlockSpec(memory_space=pltpu.VMEM)] * len(results),
        out_shape=results,
        scratch_shapes=[
            pltpu.VMEM((2 * SIDE, 3 * width, hidden), BF),
            pltpu.VMEM((SIDE, count * capacity, width), BF),
            pltpu.VMEM((count, lanes, width), BF),
            pltpu.SemaphoreType.DMA((2 * SIDE, 2)),
        ],
        compiler_params=pltpu.CompilerParams(vmem_limit_bytes=58 * 2**20),
        cost_estimate=pl.CostEstimate(
            flops=flops, bytes_accessed=moved, transcendentals=count * entries * hidden * 2
        ),
    )(*operands, *arrays)
    return [[made[to : to + n] for _, _, _, n, _, to in placed] for placed in layout]


def per_device(tokens, gain_in, expert_ids, gate_weights, w_gate, w_up, w_down, gain_out):
    rows, width = tokens.shape
    top = expert_ids.shape[1]
    members = lax.axis_size("ep")
    planes = members // SIDE
    half = planes // 2
    experts = w_gate.shape[0] * members
    capacity = 2 * rows * top // experts
    entries = SIDE * capacity
    part = width // PARTS

    def along_z(step):
        return [(i, ((i // SIDE + step) % planes) * SIDE + i % SIDE) for i in range(members)]

    def along_x(step):
        return [(i, (i // SIDE) * SIDE + (i % SIDE + step) % SIDE) for i in range(members)]

    bound = [min(rows, entries * (half - h) + entries // 2) for h in range(1, half + 1)]

    me = lax.axis_index("ep")
    core = lax.axis_index("tp")
    my_z, my_x = me // SIDE, me % SIDE

    ids = lax.dynamic_slice_in_dim(expert_ids, core * rows, rows, 0)
    gates = lax.dynamic_slice_in_dim(gate_weights, core * rows, rows, 0)
    flat = ids.reshape(-1)
    slot = pair_slots(flat)
    ahead = jnp.mod(flat // SIDE - my_z, planes)
    beside = jnp.mod(flat % SIDE - my_x, SIDE)
    upper = slot < capacity // 2
    up_reach = jnp.where((ahead < half) | ((ahead == half) & upper), ahead, 0)
    down_reach = jnp.where((ahead > half) | ((ahead == half) & ~upper), planes - ahead, 0)
    ranks = [far_first(jnp.max(r.reshape(rows, top), axis=1)) for r in (up_reach, down_reach)]
    column = ahead * entries + beside * capacity + slot
    flat_gates = gates.reshape(-1)
    gate_hi = flat_gates.astype(BF)
    gate_lo = (flat_gates - gate_hi.astype(F32)).astype(BF)
    values = jnp.stack(
        [jnp.repeat(r, top).astype(BF) for r in (ranks[0], ranks[1], jnp.arange(rows))]
        + [gate_hi, gate_lo, jnp.ones_like(gate_hi)],
        axis=1,
    )
    chosen = (jnp.arange(planes * entries)[:, None] == column[None, :]).astype(BF)
    table = dot(chosen, values).reshape(planes, entries, values.shape[1])
    filled = table[:, :, 5] > 0
    low_slot = (jnp.arange(entries) % capacity) < capacity // 2

    def routing(index, gate):
        twice = jnp.concatenate([index, index], axis=1).reshape(-1)
        return jnp.pad(jnp.stack([twice, gate.reshape(-1)]).astype(BF), ((0, HEAD - 2), (0, 0)))

    def header(direction):
        planes_of = [h if direction == 0 else planes - h for h in range(1, half + 1)]
        index = jnp.stack([table[p, :, direction] for p in planes_of])
        ok = jnp.stack([filled[p] for p in planes_of])
        last = low_slot if direction == 0 else ~low_slot
        ok = ok.at[half - 1].set(ok[half - 1] & last)
        gate = jnp.concatenate(
            [jnp.stack([table[p, :, column] for p in planes_of]) for column in (3, 4)], axis=1
        )
        return routing(jnp.where(ok, index, NOWHERE), gate)

    x_float = tokens.astype(F32)
    normed = (x_float * rms(x_float) * gain_in).astype(BF)

    orders = [(jnp.arange(rows)[:, None] == r[None, :]).astype(BF) for r in ranks]
    buffers = []
    for d in (0, 1):
        ordered = dot(orders[d], normed, BF)
        pieces = [ordered[:, p * part : (p + 1) * part] for p in range(PARTS)]
        pieces[0] = jnp.concatenate([header(d), pieces[0]], axis=0)
        buffers.append(pieces)

    swap = [(0, 1), (1, 0)]

    packed = jnp.concatenate([w_gate[0], w_up[0], w_down[0]], axis=0)
    split = packed.shape[0] // 2
    from_left = lax.ppermute(packed, "ep", along_x(1))
    from_right = lax.ppermute(packed, "ep", along_x(-1))
    far_top = lax.ppermute(from_left[:split], "ep", along_x(1))
    far_low = lax.ppermute(from_right[split:], "ep", along_x(-1))
    weights = []
    for array in (packed, from_right, (far_top, far_low), from_left):
        if isinstance(array, tuple):
            mine = [(a, 0) for a in array]
            other = [(lax.ppermute(a, "tp", swap), 0) for a in array]
        else:
            mine = [(array, 0), (array, split)]
            swapped = lax.ppermute(array, "tp", swap)
            other = [(swapped, 0), (swapped, split)]
        weights.append((mine, other))

    own_index = jnp.where(filled[0], table[0, :, 2], NOWHERE)
    own_gate = jnp.concatenate([table[0, :, 3], table[0, :, 4]])
    own_route = routing(own_index[None], own_gate[None])
    arrived = {0: [[(own_route, 0, [normed])]]}
    for h in range(1, half + 1):
        here = []
        for d in (0, 1):
            step = 1 if d == 0 else -1
            got = []
            for p in range(PARTS):
                take = bound[h - 1] + (HEAD if p == 0 else 0)
                got.append(lax.ppermute(buffers[d][p][:take], "ep", along_z(step)))
            buffers[d] = got
            here.append((None, h, got))
        arrived[h] = [here] if h == half else [[one] for one in here]

    answers = {}
    for batch in BATCHES:
        made = plane_experts([s for h in batch for s in arrived[h]], weights, capacity, width)
        for h in batch:
            answers[h] = [one for _ in arrived[h] for one in made.pop(0)]

    carried = [None, None]
    for h in range(half, 0, -1):
        for d in (0, 1):
            step = -1 if d == 0 else 1
            local = answers[h][d]
            if carried[d] is not None:
                extra = bound[h - 1] - carried[d][0].shape[0]
                local = [
                    (mine.astype(F32) + jnp.pad(c.astype(F32), ((0, extra), (0, 0)))).astype(BF)
                    for mine, c in zip(local, carried[d])
                ]
            carried[d] = [lax.ppermute(one, "ep", along_z(step)) for one in local]

    back = jnp.concatenate(orders, axis=0)
    outs = [
        dot_t(back, jnp.concatenate([carried[0][p], carried[1][p]], axis=0)) for p in range(PARTS)
    ]
    combined = jnp.concatenate(outs, axis=1) + answers[0][0][0].astype(F32)
    scaled = (combined * rms(combined)).astype(BF)
    share = width // 2
    keep = lax.dynamic_slice_in_dim(scaled, core * share, share, 1)
    give = lax.dynamic_slice_in_dim(scaled, (1 - core) * share, share, 1)
    got = lax.ppermute(give, "tp", swap)
    first = jnp.where(core == 0, keep, got)
    second = jnp.where(core == 0, got, keep)
    both = jnp.concatenate([first, second], axis=0).astype(F32)
    return (both * gain_out).astype(BF)


def solution(mesh):
    placed = (
        P(("grp", "ep", "tp"), None),
        P(),
        P(("grp", "ep"), None),
        P(("grp", "ep"), None),
        P("ep", None, "tp"),
        P("ep", None, "tp"),
        P("ep", None, "tp"),
        P("tp"),
    )

    return jax.shard_map(
        per_device, mesh=mesh, in_specs=placed, out_specs=P(("grp", "ep"), "tp"), check_vma=False
    )
```

```python
import jax
import jax.numpy as jnp
from jax import lax
from jax.experimental import pallas as pl
from jax.experimental.pallas import tpu as pltpu
from jax.sharding import PartitionSpec as P


EPS = 1e-06
SIDE = 4
PARTS = 2
WEIGHTS_IN = pltpu.HBM
NOWHERE = -128.0
HEAD = 8
BATCHES = ((5, 6, 7, 8), (3, 4), (0, 1, 2))
BF = jnp.bfloat16
F32 = jnp.float32


def dot(a, b, out=F32):
    return jnp.dot(a, b, preferred_element_type=F32).astype(out)


def dot_t(a, b):
    return lax.dot_general(a, b, (((0,), (0,)), ((), ())), preferred_element_type=F32)


def rms(x):
    return lax.rsqrt(jnp.mean(x * x, axis=1, keepdims=True) + EPS)


def pair_slots(experts_of):
    number = experts_of.shape[0]
    same = experts_of[:, None] == experts_of[None, :]
    earlier = jnp.arange(number)[:, None] > jnp.arange(number)[None, :]
    return jnp.sum((same & earlier).astype(jnp.int32), axis=1)


def far_first(reach):
    number = reach.shape[0]
    order = jnp.arange(number)
    ahead = (reach[None, :] > reach[:, None]) | (
        (reach[None, :] == reach[:, None]) & (order[None, :] < order[:, None])
    )
    return jnp.sum(ahead.astype(jnp.int32), axis=1)


def plane_experts(sources, weights, capacity, width):
    count = len(sources)
    entries = SIDE * capacity
    lanes = 2 * entries
    operands, layout, results = [], [], []
    for source in sources:
        placed = []
        for routing, distance, parts in source:
            at = len(operands)
            operands.extend(([] if routing is None else [routing]) + list(parts))
            number = parts[-1].shape[0]
            placed.append((at, routing is None, distance, len(parts), number, len(results)))
            results.extend(jax.ShapeDtypeStruct((number, p.shape[1]), BF) for p in parts)
        layout.append(placed)
    arrays, pieces = [], []
    for e, pair in enumerate(weights):
        for k, parts in enumerate(pair):
            for i, (array, at) in enumerate(parts):
                known = [n for n, a in enumerate(arrays) if a is array]
                if not known:
                    arrays.append(array)
                pieces.append((2 * e + k, i, known[0] if known else len(arrays) - 1, at))
    hidden = arrays[0].shape[1]
    part_rows = 3 * width // 2

    def body(*refs):
        ins = refs[: len(operands)]
        held = refs[len(operands) : len(operands) + len(arrays)]
        outs = refs[len(operands) + len(arrays) : -4]
        store, rows, answers, sems = refs[-4:]
        for slot, i, n, at in pieces:
            pltpu.make_async_copy(
                held[n].at[at : at + part_rows],
                store.at[slot, i * part_rows : (i + 1) * part_rows],
                sems.at[slot, i],
            ).start()

        def routed(at, inside, distance, number):
            if inside:
                lane = (distance - 1) * lanes
                head = ins[at][0:HEAD, lane : lane + lanes].astype(F32)
            else:
                head = ins[at][...].astype(F32)
            place = lax.broadcasted_iota(jnp.int32, (number, lanes), 0).astype(F32)
            return head, place == head[0:1]

        for i, source in enumerate(layout):
            total = None
            for at, inside, distance, parts, number, _ in source:
                _, hot = routed(at, inside, distance, number)
                pick = jnp.where(hot, 1.0, 0.0)
                found = []
                for p in range(parts):
                    values = ins[at + (0 if inside else 1) + p]
                    choice = pick
                    if inside and p == 0:
                        choice = jnp.concatenate([jnp.zeros((HEAD, lanes), F32), pick], axis=0)
                    found.append(
                        lax.dot_general(
                            choice.astype(BF),
                            values[...],
                            (((0,), (0,)), ((), ())),
                            preferred_element_type=F32,
                        )[:entries]
                    )
                found = jnp.concatenate(found, axis=1) if parts > 1 else found[0]
                total = found if total is None else total + found
            total = total.astype(BF)
            for e in range(SIDE):
                rows[e, i * capacity : (i + 1) * capacity, :] = total[
                    e * capacity : (e + 1) * capacity
                ]

        def one_expert(e, carry):
            x = rows[e]
            y = None
            for k in (0, 1):
                slot = 2 * e + k
                for i in (0, 1):
                    pltpu.make_async_copy(
                        held[0].at[:part_rows],
                        store.at[slot, i * part_rows : (i + 1) * part_rows],
                        sems.at[slot, i],
                    ).wait()
                g = jnp.dot(x, store[slot, :width], preferred_element_type=F32)
                u = jnp.dot(x, store[slot, width : 2 * width], preferred_element_type=F32)
                h = (g / (1.0 + jnp.exp(-g)) * u).astype(BF)
                part = lax.dot_general(
                    h,
                    store[slot, 2 * width :],
                    (((1,), (1,)), ((), ())),
                    preferred_element_type=F32,
                )
                y = part if y is None else y + part
            y = y.astype(BF)
            for i in range(count):
                mine = y[i * capacity : (i + 1) * capacity]
                for base in (0, entries):
                    first = pl.multiple_of(base + e * capacity, capacity)
                    answers[i, pl.ds(first, capacity), :] = mine
            return carry

        lax.fori_loop(0, SIDE, one_expert, 0)

        for i, source in enumerate(layout):
            for at, inside, distance, parts, number, to in source:
                head, hot = routed(at, inside, distance, number)
                spread = jnp.where(hot, head[1:2], 0.0).astype(BF)
                lane = 0
                for p in range(parts):
                    span = outs[to + p].shape[1]
                    outs[to + p][...] = jnp.dot(
                        spread, answers[i, :, lane : lane + span], preferred_element_type=F32
                    ).astype(BF)
                    lane += span

    flops = count * entries * width * hidden * 12
    moved = 2 * width * hidden * 6 * SIDE + sum(a.size * 4 for a in operands)
    made = pl.pallas_call(
        body,
        in_specs=[pl.BlockSpec(memory_space=pltpu.VMEM)] * len(operands)
        + [pl.BlockSpec(memory_space=WEIGHTS_IN)] * len(arrays),
        out_specs=[pl.BlockSpec(memory_space=pltpu.VMEM)] * len(results),
        out_shape=results,
        scratch_shapes=[
            pltpu.VMEM((2 * SIDE, 3 * width, hidden), BF),
            pltpu.VMEM((SIDE, count * capacity, width), BF),
            pltpu.VMEM((count, lanes, width), BF),
            pltpu.SemaphoreType.DMA((2 * SIDE, 2)),
        ],
        compiler_params=pltpu.CompilerParams(vmem_limit_bytes=58 * 2**20),
        cost_estimate=pl.CostEstimate(
            flops=flops, bytes_accessed=moved, transcendentals=count * entries * hidden * 2
        ),
    )(*operands, *arrays)
    return [[made[to : to + n] for _, _, _, n, _, to in placed] for placed in layout]


def per_device(tokens, gain_in, expert_ids, gate_weights, w_gate, w_up, w_down, gain_out):
    rows, width = tokens.shape
    top = expert_ids.shape[1]
    members = lax.axis_size("ep")
    planes = members // SIDE
    half = planes // 2
    experts = w_gate.shape[0] * members
    capacity = 2 * rows * top // experts
    entries = SIDE * capacity
    part = width // PARTS

    def along_z(step):
        return [(i, ((i // SIDE + step) % planes) * SIDE + i % SIDE) for i in range(members)]

    def along_x(step):
        return [(i, (i // SIDE) * SIDE + (i % SIDE + step) % SIDE) for i in range(members)]

    bound = [min(rows, entries * (half - h) + entries // 2) for h in range(1, half + 1)]

    me = lax.axis_index("ep")
    core = lax.axis_index("tp")
    my_z, my_x = me // SIDE, me % SIDE

    ids = lax.dynamic_slice_in_dim(expert_ids, core * rows, rows, 0)
    gates = lax.dynamic_slice_in_dim(gate_weights, core * rows, rows, 0)
    flat = ids.reshape(-1)
    slot = pair_slots(flat)
    ahead = jnp.mod(flat // SIDE - my_z, planes)
    beside = jnp.mod(flat % SIDE - my_x, SIDE)
    upper = slot < capacity // 2
    up_reach = jnp.where((ahead < half) | ((ahead == half) & upper), ahead, 0)
    down_reach = jnp.where((ahead > half) | ((ahead == half) & ~upper), planes - ahead, 0)
    ranks = [far_first(jnp.max(r.reshape(rows, top), axis=1)) for r in (up_reach, down_reach)]
    column = ahead * entries + beside * capacity + slot
    flat_gates = gates.reshape(-1)
    gate_hi = flat_gates.astype(BF)
    gate_lo = (flat_gates - gate_hi.astype(F32)).astype(BF)
    values = jnp.stack(
        [jnp.repeat(r, top).astype(BF) for r in (ranks[0], ranks[1], jnp.arange(rows))]
        + [gate_hi, gate_lo, jnp.ones_like(gate_hi)],
        axis=1,
    )
    chosen = (jnp.arange(planes * entries)[:, None] == column[None, :]).astype(BF)
    table = dot(chosen, values).reshape(planes, entries, values.shape[1])
    filled = table[:, :, 5] > 0
    low_slot = (jnp.arange(entries) % capacity) < capacity // 2

    def routing(index, gate):
        twice = jnp.concatenate([index, index], axis=1).reshape(-1)
        return jnp.pad(jnp.stack([twice, gate.reshape(-1)]).astype(BF), ((0, HEAD - 2), (0, 0)))

    def header(direction):
        planes_of = [h if direction == 0 else planes - h for h in range(1, half + 1)]
        index = jnp.stack([table[p, :, direction] for p in planes_of])
        ok = jnp.stack([filled[p] for p in planes_of])
        last = low_slot if direction == 0 else ~low_slot
        ok = ok.at[half - 1].set(ok[half - 1] & last)
        gate = jnp.concatenate(
            [jnp.stack([table[p, :, column] for p in planes_of]) for column in (3, 4)], axis=1
        )
        return routing(jnp.where(ok, index, NOWHERE), gate)

    x_float = tokens.astype(F32)
    normed = (x_float * rms(x_float) * gain_in).astype(BF)

    orders = [(jnp.arange(rows)[:, None] == r[None, :]).astype(BF) for r in ranks]
    buffers = []
    for d in (0, 1):
        ordered = dot(orders[d], normed, BF)
        pieces = [ordered[:, p * part : (p + 1) * part] for p in range(PARTS)]
        pieces[0] = jnp.concatenate([header(d), pieces[0]], axis=0)
        buffers.append(pieces)

    swap = [(0, 1), (1, 0)]

    packed = jnp.concatenate([w_gate[0], w_up[0], w_down[0]], axis=0)
    split = packed.shape[0] // 2
    from_left = lax.ppermute(packed, "ep", along_x(1))
    from_right = lax.ppermute(packed, "ep", along_x(-1))
    upper_rows, lower_rows = from_left[:split], from_right[split:]
    far_top = lax.ppermute(upper_rows, "ep", along_x(1))
    far_low = lax.ppermute(lower_rows, "ep", along_x(-1))
    weights = []
    for array in (packed, from_right, (far_top, far_low), from_left):
        if isinstance(array, tuple):
            mine = [(a, 0) for a in array]
            other = [(lax.ppermute(a, "tp", swap), 0) for a in array]
        else:
            mine = [(array, 0), (array, split)]
            swapped = lax.ppermute(array, "tp", swap)
            other = [(swapped, 0), (swapped, split)]
        weights.append((mine, other))

    own_index = jnp.where(filled[0], table[0, :, 2], NOWHERE)
    own_gate = jnp.concatenate([table[0, :, 3], table[0, :, 4]])
    own_route = routing(own_index[None], own_gate[None])
    arrived = {0: [[(own_route, 0, [normed])]]}
    for h in range(1, half + 1):
        here = []
        for d in (0, 1):
            step = 1 if d == 0 else -1
            got = []
            for p in range(PARTS):
                take = bound[h - 1] + (HEAD if p == 0 else 0)
                ahead_rows = buffers[d][p][:take]
                got.append(lax.ppermute(ahead_rows, "ep", along_z(step)))
            buffers[d] = got
            here.append((None, h, got))
        arrived[h] = [here] if h == half else [[one] for one in here]

    answers = {}
    for batch in BATCHES:
        made = plane_experts([s for h in batch for s in arrived[h]], weights, capacity, width)
        for h in batch:
            answers[h] = [one for _ in arrived[h] for one in made.pop(0)]

    carried = [None, None]
    for h in range(half, 0, -1):
        for d in (0, 1):
            step = -1 if d == 0 else 1
            local = answers[h][d]
            if carried[d] is not None:
                extra = bound[h - 1] - carried[d][0].shape[0]
                local = [
                    (mine.astype(F32) + jnp.pad(c.astype(F32), ((0, extra), (0, 0)))).astype(BF)
                    for mine, c in zip(local, carried[d])
                ]
            carried[d] = [lax.ppermute(one, "ep", along_z(step)) for one in local]

    back = jnp.concatenate(orders, axis=0)
    outs = [
        dot_t(back, jnp.concatenate([carried[0][p], carried[1][p]], axis=0)) for p in range(PARTS)
    ]
    combined = jnp.concatenate(outs, axis=1) + answers[0][0][0].astype(F32)
    scaled = (combined * rms(combined)).astype(BF)
    share = width // 2
    keep = lax.dynamic_slice_in_dim(scaled, core * share, share, 1)
    give = lax.dynamic_slice_in_dim(scaled, (1 - core) * share, share, 1)
    got = lax.ppermute(give, "tp", swap)
    first = jnp.where(core == 0, keep, got)
    second = jnp.where(core == 0, got, keep)
    both = jnp.concatenate([first, second], axis=0).astype(F32)
    return (both * gain_out).astype(BF)


def solution(mesh):
    placed = (
        P(("grp", "ep", "tp"), None),
        P(),
        P(("grp", "ep"), None),
        P(("grp", "ep"), None),
        P("ep", None, "tp"),
        P("ep", None, "tp"),
        P("ep", None, "tp"),
        P("tp"),
    )

    return jax.shard_map(
        per_device, mesh=mesh, in_specs=placed, out_specs=P(("grp", "ep"), "tp"), check_vma=False
    )
```

```python
import jax
import jax.numpy as jnp
from jax import lax
from jax.experimental import pallas as pl
from jax.experimental.pallas import tpu as pltpu
from jax.sharding import PartitionSpec as P


EPS = 1e-06
SIDE = 4
PARTS = 2
NOWHERE = -128.0
HEAD = 8
BATCHES = ((5, 6, 7, 8), (4,), (0, 1, 2, 3))
BF = jnp.bfloat16
F32 = jnp.float32


def dot(a, b, out=F32):
    return jnp.dot(a, b, preferred_element_type=F32).astype(out)


def dot_t(a, b):
    return lax.dot_general(a, b, (((0,), (0,)), ((), ())), preferred_element_type=F32)


def rms(x):
    return lax.rsqrt(jnp.mean(x * x, axis=1, keepdims=True) + EPS)


def pair_slots(experts_of):
    number = experts_of.shape[0]
    same = experts_of[:, None] == experts_of[None, :]
    earlier = jnp.arange(number)[:, None] > jnp.arange(number)[None, :]
    return jnp.sum((same & earlier).astype(jnp.int32), axis=1)


def far_first(reach):
    number = reach.shape[0]
    order = jnp.arange(number)
    ahead = (reach[None, :] > reach[:, None]) | (
        (reach[None, :] == reach[:, None]) & (order[None, :] < order[:, None])
    )
    return jnp.sum(ahead.astype(jnp.int32), axis=1)


def plane_experts(sources, weights, capacity, width):
    count = len(sources)
    entries = SIDE * capacity
    lanes = 2 * entries
    operands, layout, results = [], [], []
    for source in sources:
        placed = []
        for routing, distance, parts in source:
            at = len(operands)
            operands.extend(([] if routing is None else [routing]) + list(parts))
            number = parts[-1].shape[0]
            placed.append((at, routing is None, distance, len(parts), number, len(results)))
            results.extend(jax.ShapeDtypeStruct((number, p.shape[1]), BF) for p in parts)
        layout.append(placed)
    arrays, pieces = [], []
    for e, pair in enumerate(weights):
        for k, parts in enumerate(pair):
            for i, (array, at) in enumerate(parts):
                known = [n for n, a in enumerate(arrays) if a is array]
                if not known:
                    arrays.append(array)
                pieces.append((2 * e + k, i, known[0] if known else len(arrays) - 1, at))
    hidden = arrays[0].shape[1]
    part_rows = 3 * width // 2

    def body(*refs):
        given = refs[: len(operands)]
        held = refs[len(operands) : len(operands) + len(arrays)]
        own = refs[len(operands) + len(arrays) : -5]
        outs, ins = own[: len(results)], own[len(results) :]
        store, rows, answers, sems, in_sems = refs[-5:]
        reads = [
            pltpu.make_async_copy(a, b, in_sems.at[i]) for i, (a, b) in enumerate(zip(given, ins))
        ]
        for copy in reads:
            copy.start()
        for slot, i, n, at in pieces:
            pltpu.make_async_copy(
                held[n].at[at : at + part_rows],
                store.at[slot, i * part_rows : (i + 1) * part_rows],
                sems.at[slot, i],
            ).start()

        def routed(at, inside, distance, number):
            if inside:
                lane = (distance - 1) * lanes
                head = ins[at][0:HEAD, lane : lane + lanes].astype(F32)
            else:
                head = ins[at][...].astype(F32)
            place = lax.broadcasted_iota(jnp.int32, (number, lanes), 0).astype(F32)
            return head, place == head[0:1]

        for i, source in enumerate(layout):
            total = None
            for at, inside, distance, parts, number, _ in source:
                for n in range(parts + (0 if inside else 1)):
                    reads[at + n].wait()
                _, hot = routed(at, inside, distance, number)
                pick = jnp.where(hot, 1.0, 0.0)
                found = []
                for p in range(parts):
                    values = ins[at + (0 if inside else 1) + p]
                    choice = pick
                    if inside and p == 0:
                        choice = jnp.concatenate([jnp.zeros((HEAD, lanes), F32), pick], axis=0)
                    found.append(
                        lax.dot_general(
                            choice.astype(BF),
                            values[...],
                            (((0,), (0,)), ((), ())),
                            preferred_element_type=F32,
                        )[:entries]
                    )
                found = jnp.concatenate(found, axis=1) if parts > 1 else found[0]
                total = found if total is None else total + found
            total = total.astype(BF)
            for e in range(SIDE):
                rows[e, i * capacity : (i + 1) * capacity, :] = total[
                    e * capacity : (e + 1) * capacity
                ]

        def one_expert(e, carry):
            x = rows[e]
            y = None
            for k in (0, 1):
                slot = 2 * e + k
                for i in (0, 1):
                    pltpu.make_async_copy(
                        held[0].at[:part_rows],
                        store.at[slot, i * part_rows : (i + 1) * part_rows],
                        sems.at[slot, i],
                    ).wait()
                g = jnp.dot(x, store[slot, :width], preferred_element_type=F32)
                u = jnp.dot(x, store[slot, width : 2 * width], preferred_element_type=F32)
                h = (g / (1.0 + jnp.exp(-g)) * u).astype(BF)
                part = lax.dot_general(
                    h,
                    store[slot, 2 * width :],
                    (((1,), (1,)), ((), ())),
                    preferred_element_type=F32,
                )
                y = part if y is None else y + part
            y = y.astype(BF)
            for i in range(count):
                mine = y[i * capacity : (i + 1) * capacity]
                for base in (0, entries):
                    first = pl.multiple_of(base + e * capacity, capacity)
                    answers[i, pl.ds(first, capacity), :] = mine
            return carry

        lax.fori_loop(0, SIDE, one_expert, 0)

        for i, source in enumerate(layout):
            for at, inside, distance, parts, number, to in source:
                head, hot = routed(at, inside, distance, number)
                spread = jnp.where(hot, head[1:2], 0.0).astype(BF)
                lane = 0
                for p in range(parts):
                    span = outs[to + p].shape[1]
                    outs[to + p][...] = jnp.dot(
                        spread, answers[i, :, lane : lane + span], preferred_element_type=F32
                    ).astype(BF)
                    lane += span

    flops = count * entries * width * hidden * 12
    moved = 2 * width * hidden * 6 * SIDE + sum(a.size * 4 for a in operands)
    made = pl.pallas_call(
        body,
        in_specs=[pl.BlockSpec(memory_space=pltpu.HBM)] * (len(operands) + len(arrays)),
        out_specs=[pl.BlockSpec(memory_space=pltpu.VMEM)] * len(results),
        out_shape=results,
        scratch_shapes=[pltpu.VMEM(a.shape, BF) for a in operands]
        + [
            pltpu.VMEM((2 * SIDE, 3 * width, hidden), BF),
            pltpu.VMEM((SIDE, count * capacity, width), BF),
            pltpu.VMEM((count, lanes, width), BF),
            pltpu.SemaphoreType.DMA((2 * SIDE, 2)),
            pltpu.SemaphoreType.DMA((len(operands),)),
        ],
        compiler_params=pltpu.CompilerParams(vmem_limit_bytes=58 * 2**20),
        cost_estimate=pl.CostEstimate(
            flops=flops, bytes_accessed=moved, transcendentals=count * entries * hidden * 2
        ),
    )(*operands, *arrays)
    return [[made[to : to + n] for _, _, _, n, _, to in placed] for placed in layout]


def per_device(tokens, gain_in, expert_ids, gate_weights, w_gate, w_up, w_down, gain_out):
    rows, width = tokens.shape
    top = expert_ids.shape[1]
    members = lax.axis_size("ep")
    planes = members // SIDE
    half = planes // 2
    experts = w_gate.shape[0] * members
    capacity = 2 * rows * top // experts
    entries = SIDE * capacity
    part = width // PARTS

    def along_z(step):
        return [(i, ((i // SIDE + step) % planes) * SIDE + i % SIDE) for i in range(members)]

    def along_x(step):
        return [(i, (i // SIDE) * SIDE + (i % SIDE + step) % SIDE) for i in range(members)]

    bound = [min(rows, entries * (half - h) + entries // 2) for h in range(1, half + 1)]

    me = lax.axis_index("ep")
    core = lax.axis_index("tp")
    my_z, my_x = me // SIDE, me % SIDE

    ids = lax.dynamic_slice_in_dim(expert_ids, core * rows, rows, 0)
    gates = lax.dynamic_slice_in_dim(gate_weights, core * rows, rows, 0)
    flat = ids.reshape(-1)
    slot = pair_slots(flat)
    ahead = jnp.mod(flat // SIDE - my_z, planes)
    beside = jnp.mod(flat % SIDE - my_x, SIDE)
    upper = slot < capacity // 2
    up_reach = jnp.where((ahead < half) | ((ahead == half) & upper), ahead, 0)
    down_reach = jnp.where((ahead > half) | ((ahead == half) & ~upper), planes - ahead, 0)
    ranks = [far_first(jnp.max(r.reshape(rows, top), axis=1)) for r in (up_reach, down_reach)]
    column = ahead * entries + beside * capacity + slot
    flat_gates = gates.reshape(-1)
    gate_hi = flat_gates.astype(BF)
    gate_lo = (flat_gates - gate_hi.astype(F32)).astype(BF)
    values = jnp.stack(
        [jnp.repeat(r, top).astype(BF) for r in (ranks[0], ranks[1], jnp.arange(rows))]
        + [gate_hi, gate_lo, jnp.ones_like(gate_hi)],
        axis=1,
    )
    chosen = (jnp.arange(planes * entries)[:, None] == column[None, :]).astype(BF)
    table = dot(chosen, values).reshape(planes, entries, values.shape[1])
    filled = table[:, :, 5] > 0
    low_slot = (jnp.arange(entries) % capacity) < capacity // 2

    def routing(index, gate):
        twice = jnp.concatenate([index, index], axis=1).reshape(-1)
        return jnp.pad(jnp.stack([twice, gate.reshape(-1)]).astype(BF), ((0, HEAD - 2), (0, 0)))

    def header(direction):
        planes_of = [h if direction == 0 else planes - h for h in range(1, half + 1)]
        index = jnp.stack([table[p, :, direction] for p in planes_of])
        ok = jnp.stack([filled[p] for p in planes_of])
        last = low_slot if direction == 0 else ~low_slot
        ok = ok.at[half - 1].set(ok[half - 1] & last)
        gate = jnp.concatenate(
            [jnp.stack([table[p, :, column] for p in planes_of]) for column in (3, 4)], axis=1
        )
        return routing(jnp.where(ok, index, NOWHERE), gate)

    x_float = tokens.astype(F32)
    normed = (x_float * rms(x_float) * gain_in).astype(BF)

    orders = [(jnp.arange(rows)[:, None] == r[None, :]).astype(BF) for r in ranks]
    buffers = []
    for d in (0, 1):
        ordered = dot(orders[d], normed, BF)
        pieces = [ordered[:, p * part : (p + 1) * part] for p in range(PARTS)]
        pieces[0] = jnp.concatenate([header(d), pieces[0]], axis=0)
        buffers.append(pieces)

    swap = [(0, 1), (1, 0)]

    packed = jnp.concatenate([w_gate[0], w_up[0], w_down[0]], axis=0)
    split = packed.shape[0] // 2
    from_left = lax.ppermute(packed, "ep", along_x(1))
    from_right = lax.ppermute(packed, "ep", along_x(-1))
    upper_rows, lower_rows = from_left[:split], from_right[split:]
    far_top = lax.ppermute(upper_rows, "ep", along_x(1))
    far_low = lax.ppermute(lower_rows, "ep", along_x(-1))
    weights = []
    for array in (packed, from_right, (far_top, far_low), from_left):
        if isinstance(array, tuple):
            mine = [(a, 0) for a in array]
            other = [(lax.ppermute(a, "tp", swap), 0) for a in array]
        else:
            mine = [(array, 0), (array, split)]
            swapped = lax.ppermute(array, "tp", swap)
            other = [(swapped, 0), (swapped, split)]
        weights.append((mine, other))

    own_index = jnp.where(filled[0], table[0, :, 2], NOWHERE)
    own_gate = jnp.concatenate([table[0, :, 3], table[0, :, 4]])
    own_route = routing(own_index[None], own_gate[None])
    arrived = {0: [[(own_route, 0, [normed])]]}
    for h in range(1, half + 1):
        here = []
        for d in (0, 1):
            step = 1 if d == 0 else -1
            got = []
            for p in range(PARTS):
                take = bound[h - 1] + (HEAD if p == 0 else 0)
                ahead_rows = buffers[d][p][:take]
                got.append(lax.ppermute(ahead_rows, "ep", along_z(step)))
            buffers[d] = got
            here.append((None, h, got))
        arrived[h] = [here] if h == half else [[one] for one in here]

    answers = {}
    for batch in BATCHES:
        made = plane_experts([s for h in batch for s in arrived[h]], weights, capacity, width)
        for h in batch:
            answers[h] = [one for _ in arrived[h] for one in made.pop(0)]

    carried = [None, None]
    for h in range(half, 0, -1):
        for d in (0, 1):
            step = -1 if d == 0 else 1
            local = answers[h][d]
            if carried[d] is not None:
                extra = bound[h - 1] - carried[d][0].shape[0]
                local = [
                    (mine.astype(F32) + jnp.pad(c.astype(F32), ((0, extra), (0, 0)))).astype(BF)
                    for mine, c in zip(local, carried[d])
                ]
            carried[d] = [lax.ppermute(one, "ep", along_z(step)) for one in local]

    back = jnp.concatenate(orders, axis=0)
    outs = [
        dot_t(back, jnp.concatenate([carried[0][p], carried[1][p]], axis=0)) for p in range(PARTS)
    ]
    combined = jnp.concatenate(outs, axis=1) + answers[0][0][0].astype(F32)
    scaled = (combined * rms(combined)).astype(BF)
    share = width // 2
    keep = lax.dynamic_slice_in_dim(scaled, core * share, share, 1)
    give = lax.dynamic_slice_in_dim(scaled, (1 - core) * share, share, 1)
    got = lax.ppermute(give, "tp", swap)
    first = jnp.where(core == 0, keep, got)
    second = jnp.where(core == 0, got, keep)
    both = jnp.concatenate([first, second], axis=0).astype(F32)
    return (both * gain_out).astype(BF)


def solution(mesh):
    placed = (
        P(("grp", "ep", "tp"), None),
        P(),
        P(("grp", "ep"), None),
        P(("grp", "ep"), None),
        P("ep", None, "tp"),
        P("ep", None, "tp"),
        P("ep", None, "tp"),
        P("tp"),
    )

    return jax.shard_map(
        per_device, mesh=mesh, in_specs=placed, out_specs=P(("grp", "ep"), "tp"), check_vma=False
    )
```
